32 devices in a mesh: ep: 4 (over y, x), tp: 8 (over z, core).
Axes of the slice: x: 2, y: 2, z: 4, core: 2. Of those that a mesh axis runs over, the one named last changes fastest.
Arguments:
- tokens: bfloat16 [64, 2048], P('ep', 'tp'), may hold values from -6 to 6
- key_cache: bfloat16 [64, 16, 1024, 128], P('ep', 'tp'), may hold values from -1700 to 1700
- value_cache: bfloat16 [64, 16, 1024, 128], P('ep', 'tp'), may hold values from -6 to 6
- gate_totals: float32 [64, 16, 1024], P('ep', 'tp'), as said below
- lengths: int32 [64], P('ep'), may hold values from 128 to 1024
- attn_gain: float32 [2048], replicated, may hold values from 0.1 to 1.9
- w_query: bfloat16 [2048, 2048], P(None, 'tp'), may hold values from -0.125 to 0.125
- w_key: bfloat16 [2048, 2048], P(None, 'tp'), may hold values from -0.125 to 0.125
- w_value: bfloat16 [2048, 2048], P(None, 'tp'), may hold values from -0.125 to 0.125
- w_forget: bfloat16 [2048, 16], replicated, may hold values from -0.125 to 0.125
- forget_bias: float32 [16], replicated, may hold values from -3 to 0
- w_attn_out: bfloat16 [2048, 2048], P('tp'), may hold values from -0.1875 to 0.1875
- moe_gain: float32 [2048], replicated, may hold values from 0.1 to 1.9
- group_ids: int32 [64, 1], P('ep'), may hold values from 0 to 3; in each aligned block of 16 rows (0 to 15, 16 to 31, ...) at most 8 rows name the same one
- inner_ids: int32 [64, 2], P('ep'), may hold values from 0 to 3, all different within a row
- group_prob: float32 [64], P('ep'), may hold values from 0.2 to 1
- pair_logits: float32 [64, 2], P('ep'), may hold values from -6 to 6
- w_expert_gate: bfloat16 [4, 2048, 2048], P('ep', None, 'tp'), may hold values from -0.125 to 0.125
- w_expert_up: bfloat16 [4, 2048, 2048], P('ep', None, 'tp'), may hold values from -0.125 to 0.125
- w_expert_down: bfloat16 [4, 2048, 2048], P('ep', 'tp'), may hold values from -0.375 to 0.375
- w_dense_in: bfloat16 [2048, 2048], P(None, 'tp'), may hold values from -0.125 to 0.125
- w_dense_out: bfloat16 [2048, 2048], P('tp'), may hold values from -0.1875 to 0.1875
- dense_gate: float32 [2048], P('tp'), may hold values from -2 to 2
Outputs:
- layer_output: bfloat16 [64, 2048], P('ep', 'tp')
- new_keys: bfloat16 [64, 16, 128], P('ep', 'tp')
- new_values: bfloat16 [64, 16, 128], P('ep', 'tp')
- new_gates: float32 [64, 16], P('ep', 'tp')
The draws below stay inside these ranges and needn't reach their ends.
Inputs may be any that keep to these rules, and one draw needn't show every extreme that they name: `group_ids`: within the 16 sequences of each index of ep (aligned blocks of rows), no group is named by more than 8 sequences, a bound that some block reaches. `inner_ids`: each row names 2 different experts of its group. `gate_totals`: along positions the values of each sequence and head never rise.
All inputs are finite; a program needn't handle non-finite values.
Results may differ from the reference program's by a relative error of at most 0.011.
Values may be sent and summed in bfloat16 or wider, within the bound.
A program may use at most 64 MiB of HBM per device.

```python
import math
import jax
import jax.numpy as jnp
import numpy as np
from jax import lax

D = 2048
HEADS = 16
HEAD_DIM = 128
FFE = 512
EPG = 4
TOPK = 2
FFD = 2048
SEQ_GRP = 16
STORED_ENTRIES = 1024
STREAM_COUNT = 64
GROUPS = 4
CAP = 8
N_EP = 4


def draw_key_cache(key, part):
    full_shape = (STREAM_COUNT, HEADS, STORED_ENTRIES, HEAD_DIM)
    base_draw = jnp.clip(jax.random.normal(jax.random.fold_in(key, 11), full_shape, jnp.float32), -5.0, 5.0)
    return base_draw.astype(jnp.bfloat16)


def draw_gate_totals(key, part):
    noise_child_seeds = jax.random.split(jax.random.fold_in(key, 21), 7)
    slow_share = 0.5
    gradual_zone_flags = jax.random.uniform(noise_child_seeds[0], (1, HEADS, 1), jnp.float32) < slow_share
    slow_total = jax.random.uniform(noise_child_seeds[1], (STREAM_COUNT, HEADS, 1), jnp.float32, 0.2, 0.7)
    fast_span = jax.random.uniform(noise_child_seeds[2], (1, HEADS, 1), jnp.float32, 30.0, 100.0)
    seq_factor = jnp.exp(jax.random.uniform(noise_child_seeds[3], (STREAM_COUNT, 1, 1), jnp.float32, 0.0, math.log(2.0)))
    rough_mult = jax.random.uniform(noise_child_seeds[4], (STREAM_COUNT, HEADS, STORED_ENTRIES), jnp.float32, 0.5, 1.5)
    fading_per_tick = jnp.where(gradual_zone_flags, slow_total / STORED_ENTRIES, 1.0 / fast_span) * seq_factor * rough_mult
    spike_index_point = jax.random.randint(noise_child_seeds[5], (STREAM_COUNT, 1, 1, 2), 0, STORED_ENTRIES)
    entry_indices = jnp.arange(STORED_ENTRIES)[None, None, :, None]
    spike_zone_flags = jnp.any(entry_indices == spike_index_point, axis=-1)
    keeping_logarithm_multiplier = jnp.log(jax.random.uniform(noise_child_seeds[6], (STREAM_COUNT, HEADS, 1), jnp.float32, 0.55, 0.8))
    logarithm_fading_tick = -fading_per_tick + jnp.where(spike_zone_flags & gradual_zone_flags, keeping_logarithm_multiplier, 0.0)
    return jnp.cumsum(logarithm_fading_tick, axis=-1)


def set_ends(array, rng, low, top_value):
    extent = array.shape
    index_at = [jax.random.randint(jax.random.fold_in(rng, axis), (), 0, extent[axis]) for axis in range(len(extent))]
    array = array.at[tuple(index_at)].set(low)
    longest = extent.index(max(extent))
    index_at[longest] = (index_at[longest] + 1) % extent[longest]
    return array.at[tuple(index_at)].set(top_value)


def strengthened(entries, stream_key, source, target, parts, factor):
    def block_of(dim):
        return (jnp.arange(entries.shape[dim]) // (entries.shape[dim] // parts)).reshape((-1,) + (1,) * (entries.ndim - 1 - dim))

    one_side = jax.random.permutation(stream_key, parts)[block_of(target)]
    other_side = (block_of(target) + parts // 2) % parts
    return jnp.where((block_of(source) == one_side) | (block_of(source) == other_side), factor * entries, entries)


def level_of(rng, dims, cuts, least, high):
    loudness = 1.0
    for axis_at, parts in cuts:
        steps = jax.random.uniform(jax.random.fold_in(jax.random.fold_in(rng, 6), axis_at), (parts,), jnp.float32, least / len(cuts), high / len(cuts))
        loudness = loudness * jnp.repeat(jnp.exp(steps), dims[axis_at] // parts).reshape((-1,) + (1,) * (len(dims) - 1 - axis_at))
    return loudness


def choose_distinct(rng, rows, number_of, top, lift):
    sequence = jax.random.permutation(jax.random.fold_in(rng, 1), number_of)
    pull = sequence
    for power in range(3):
        pull = pull * pull // number_of
    pull = pull * lift // number_of
    lots = jax.random.randint(jax.random.fold_in(rng, 2), (rows, number_of), 0, 4096) + pull
    sure = jax.random.permutation(jax.random.fold_in(rng, 3), rows)[jnp.arange(number_of) % rows]
    lots = jnp.where(jnp.arange(rows)[:, None] == sure[None, :], 1 << 14, lots)
    score = lots * number_of + jnp.arange(number_of)
    return lax.top_k(score.astype(jnp.int32), top)[1].astype(jnp.int32)


def shared_out(rng, own, number, rows, number_of, top, bound, lean):
    sequence = jax.random.permutation(rng, number_of)
    crowded, common = portions_of(number_of, rows * top, bound, lean, True), portions_of(number_of, rows * top, bound, lean, False)
    places = jnp.arange(number_of)

    def named(sizes, rotation):
        used = int((sizes > 0).sum())
        fixed = max(1, used // 4)
        shifted = fixed + (places - fixed + rotation * (used - fixed)) % max(1, number_of - fixed)
        return jnp.zeros((number_of,), jnp.int32).at[sequence[jnp.where(places < fixed, places, shifted)]].set(jnp.asarray(sizes, jnp.int32))

    sizes = jnp.where(number % 4 == 0, named(crowded, number // 4), named(common, number - number // 4 - 1))
    mixed = jax.random.permutation(jax.random.fold_in(own, 3), number_of)
    donor, sink = mixed[0:number_of // 2 * 2:2], mixed[1:number_of // 2 * 2:2]
    margin = jnp.minimum(sizes[donor] - 1, bound - sizes[sink]) // 2
    margin = jnp.where((donor == sequence[0]) | (sink == sequence[0]) | (sizes[sink] == 0), 0, jnp.maximum(margin, 0))
    shifted = jax.random.randint(jax.random.fold_in(own, 4), (number_of // 2,), 0, 1 << 20) % (margin + 1)
    sizes = sizes.at[donor].add(-shifted).at[sink].add(shifted)
    items = jnp.searchsorted(jnp.cumsum(sizes), jnp.arange(rows * top), side="right").astype(jnp.int32)
    listing = items.reshape(top, rows).T
    listing = listing[jax.random.permutation(jax.random.fold_in(own, 1), rows)]
    rotation = jax.random.randint(jax.random.fold_in(own, 2), (rows, 1), 0, top)
    return jnp.take_along_axis(listing, (jnp.arange(top)[None, :] + rotation) % top, axis=1)


def portions_of(number_of, total, limit, slope, full):
    weights = [(1 << 20) // math.isqrt(standing ** slope) + 1 for standing in range(1, number_of + 1)]
    largest = limit if full else min(limit, max(-(-total // number_of), total * weights[0] // sum(weights)))
    least = 1 if total - largest >= number_of - 1 else 0
    given, spare = [largest] + [least] * (number_of - 1), total - largest - least * (number_of - 1)
    while spare > 0:
        candidates = [i for i in range(1, number_of) if given[i] < largest] or [i for i in range(1, number_of) if given[i] < limit]
        mass, left = sum([weights[i] for i in candidates]), spare
        for i in candidates:
            addition = min(limit - given[i], max(1, left * weights[i] // mass), spare)
            given[i] = given[i] + addition
            spare = spare - addition
    return np.array(given)


def noise(own_key, shape, deviation, bound, cuts=(), kind=jnp.bfloat16):
    loudness = level_of(own_key, shape, cuts, -0.22, 0.18) if cuts else 1.0
    values = jax.random.normal(own_key, shape, jnp.float32) * deviation * loudness
    return jnp.minimum(jnp.maximum(values, -bound), bound).astype(kind)


def noise_with(stream_key, dims, scale, bound, cuts, heavy, kind=jnp.bfloat16):
    values = scale * jax.random.normal(stream_key, dims, jnp.float32)
    if cuts:
        values = values * level_of(stream_key, dims, cuts, -0.22, 0.18)
    return jnp.clip(strengthened(values, jax.random.fold_in(stream_key, 3), *heavy), -bound, bound).astype(kind)


def setup_inputs(seed: int = 0) -> dict:
    key_list = jax.random.split(jax.random.key(seed), 24)
    tokens = noise(key_list[0], (STREAM_COUNT, D), 1.0, 6.0, ((0, 4), (1, 8)))
    key_cache = draw_key_cache(jax.random.fold_in(key_list[23], 71), 0)
    value_cache = noise(key_list[2], (STREAM_COUNT, HEADS, STORED_ENTRIES, HEAD_DIM), 1.0, 6.0, ((0, 4), (1, 8)))
    gate_totals = draw_gate_totals(jax.random.fold_in(key_list[23], 71), 0)
    lengths = set_ends(jax.random.randint(key_list[4], (STREAM_COUNT,), STORED_ENTRIES // 8, STORED_ENTRIES + 1), jax.random.fold_in(key_list[4], 1), STORED_ENTRIES // 8, STORED_ENTRIES).astype(jnp.int32)
    attn_gain = jnp.clip(1.0 + 0.18 * jax.random.normal(key_list[5], (D,), jnp.float32), 0.1, 1.9)
    w_query = noise(key_list[6], (D, HEADS * HEAD_DIM), D ** -0.5, 0.125, ((1, 8),))
    w_key = noise(key_list[7], (D, HEADS * HEAD_DIM), D ** -0.5, 0.125, ((1, 8),))
    w_value = noise(key_list[8], (D, HEADS * HEAD_DIM), D ** -0.5, 0.125, ((1, 8),))
    w_forget = noise(key_list[9], (D, HEADS), D ** -0.5, 0.125)
    forget_bias = jnp.clip(jax.random.uniform(key_list[10], (HEADS,), jnp.float32, -3.0, 0.0), -3.0, 0.0)
    w_attn_out = noise_with(key_list[11], (HEADS * HEAD_DIM, D), (HEADS * HEAD_DIM) ** -0.5, 0.1875, ((0, 8),), (0, 1, 8, 2.0))
    moe_gain = jnp.clip(1.0 + 0.18 * jax.random.normal(key_list[12], (D,), jnp.float32), 0.1, 1.9)
    group_ids_keys = jax.random.split(jax.random.fold_in(key_list[13], 1), STREAM_COUNT // SEQ_GRP)
    group_ids_turns = jax.random.permutation(jax.random.fold_in(key_list[13], 3), STREAM_COUNT // SEQ_GRP)
    group_ids = jax.vmap(lambda own, number: shared_out(jax.random.fold_in(key_list[13], 2), own, number, SEQ_GRP, N_EP, 1, CAP, 1))(group_ids_keys, group_ids_turns).reshape((STREAM_COUNT, 1))
    inner_ids = choose_distinct(key_list[14], STREAM_COUNT, EPG, TOPK, 0)
    group_prob = jnp.clip(0.2 + 0.8 * jax.random.uniform(key_list[15], (STREAM_COUNT,), jnp.float32) ** level_of(key_list[15], (STREAM_COUNT,), ((0, 4),), -0.2, 0.2), 0.2, 1.0)
    pair_logits = noise(key_list[16], (STREAM_COUNT, TOPK), 1.5, 6.0, ((0, 4),), jnp.float32)
    w_expert_gate = noise(key_list[17], (GROUPS, D, EPG * FFE), D ** -0.5, 0.125, ((0, 4), (2, 8)))
    w_expert_up = noise(key_list[18], (GROUPS, D, EPG * FFE), D ** -0.5, 0.125, ((0, 4), (2, 8)))
    w_expert_down = noise_with(key_list[19], (GROUPS, EPG * FFE, D), FFE ** -0.5, 0.375, ((0, 4), (1, 8)), (1, 2, 8, 2.0))
    w_dense_in = noise(key_list[20], (D, FFD), D ** -0.5, 0.125, ((1, 8),))
    w_dense_out = noise_with(key_list[21], (FFD, D), FFD ** -0.5, 0.1875, ((0, 8),), (0, 1, 8, 2.0))
    dense_gate = jnp.clip(jax.random.uniform(key_list[22], (D,), jnp.float32, -2.0, 2.0) * level_of(key_list[22], (D,), ((0, 8),), -0.4, 0.0), -2.0, 2.0)
    return {"tokens": tokens, "key_cache": key_cache, "value_cache": value_cache, "gate_totals": gate_totals, "lengths": lengths, "attn_gain": attn_gain, "w_query": w_query, "w_key": w_key, "w_value": w_value, "w_forget": w_forget, "forget_bias": forget_bias, "w_attn_out": w_attn_out, "moe_gain": moe_gain, "group_ids": group_ids, "inner_ids": inner_ids, "group_prob": group_prob, "pair_logits": pair_logits, "w_expert_gate": w_expert_gate, "w_expert_up": w_expert_up, "w_expert_down": w_expert_down, "w_dense_in": w_dense_in, "w_dense_out": w_dense_out, "dense_gate": dense_gate}


EPS = 1e-06
FLOOR = -1e+30

def norm_rows(row_data, gain_vec):
    values = row_data.astype(jnp.float32)
    factor = lax.rsqrt(lax.optimization_barrier(jnp.mean(values * values, axis=-1, keepdims=True)) + EPS)
    return (values * factor * gain_vec).astype(jnp.bfloat16)

def head_norm(values):
    factor = lax.rsqrt(lax.optimization_barrier(jnp.mean(values * values, axis=-1, keepdims=True)) + EPS)
    return (values * factor).astype(jnp.bfloat16)

def attend_one(packed):
    queries, fresh_key, fresh_value, key_rows, value_rows, totals, length, current = packed
    score_scale = HEAD_DIM ** (-0.5)
    scores = jnp.einsum('hd,hld->hl', queries.astype(jnp.float32), key_rows.astype(jnp.float32)) * score_scale
    scores = scores + current[:, None] - totals
    entry_indices = jnp.arange(STORED_ENTRIES)
    live_mask = (entry_indices < length)[None, :]
    scores = jnp.where(live_mask, scores, FLOOR)
    own_score = lax.optimization_barrier(jnp.sum(queries.astype(jnp.float32) * fresh_key.astype(jnp.float32), axis=-1)) * score_scale
    peak = jnp.maximum(lax.optimization_barrier(jnp.max(scores, axis=-1)), own_score)
    expo_terms = jnp.where(live_mask, jnp.exp(scores - peak[:, None]), 0.0)
    own_expo = jnp.exp(own_score - peak)
    denom_sum = lax.optimization_barrier(jnp.sum(expo_terms, axis=-1)) + own_expo
    weights = (expo_terms / denom_sum[:, None]).astype(jnp.bfloat16)
    own_weight = (own_expo / denom_sum).astype(jnp.bfloat16)
    attended = jnp.einsum('hl,hld->hd', weights.astype(jnp.float32), value_rows.astype(jnp.float32))
    attended = attended + own_weight.astype(jnp.float32)[:, None] * fresh_value.astype(jnp.float32)
    return attended.astype(jnp.bfloat16)

def reference(tokens, key_cache, value_cache, gate_totals, lengths, attn_gain, w_query, w_key, w_value, w_forget, forget_bias, w_attn_out, moe_gain, group_ids, inner_ids, group_prob, pair_logits, w_expert_gate, w_expert_up, w_expert_down, w_dense_in, w_dense_out, dense_gate):
    normed = norm_rows(tokens, attn_gain)
    seq_count = tokens.shape[0]

    def project(weight):
        return jnp.dot(normed, weight, preferred_element_type=jnp.float32).reshape(seq_count, HEADS, HEAD_DIM)
    queries = head_norm(project(w_query))
    new_keys = head_norm(project(w_key))
    new_values = project(w_value).astype(jnp.bfloat16)
    log_gate = jax.nn.log_sigmoid(jnp.dot(normed, w_forget, preferred_element_type=jnp.float32) + forget_bias)
    last_index = jnp.broadcast_to((lengths - 1).astype(jnp.int32)[:, None, None], (seq_count, HEADS, 1))
    last_total = jnp.take_along_axis(gate_totals, last_index, axis=2)[:, :, 0]
    new_gates = last_total + log_gate
    attended = lax.map(attend_one, (queries, new_keys, new_values, key_cache, value_cache, gate_totals, lengths, new_gates))
    projected = jnp.dot(attended.reshape(seq_count, HEADS * HEAD_DIM), w_attn_out, preferred_element_type=jnp.float32)
    residual = (tokens.astype(jnp.float32) + projected).astype(jnp.bfloat16)
    moe_in = norm_rows(residual, moe_gain)
    first_share = jax.nn.sigmoid(pair_logits[:, 0] - pair_logits[:, 1])
    pair_share = group_prob[:, None] * jnp.stack([first_share, 1.0 - first_share], axis=1)
    pair_share = lax.optimization_barrier(pair_share.astype(jnp.bfloat16)).astype(jnp.float32)
    inner_range = jnp.arange(EPG)
    spread = lax.optimization_barrier(jnp.sum(jnp.where(inner_ids[:, :, None] == inner_range[None, None, :], pair_share[:, :, None], 0.0), axis=1))

    def expert_one(packed):
        token_row, group_id, share_vec = packed
        gate_pre = jnp.dot(token_row[None, :], w_expert_gate[group_id], preferred_element_type=jnp.float32)[0]
        up_pre = jnp.dot(token_row[None, :], w_expert_up[group_id], preferred_element_type=jnp.float32)[0]
        weight_cols = jnp.repeat(share_vec, FFE)
        hidden = (jax.nn.silu(gate_pre) * up_pre * weight_cols).astype(jnp.bfloat16)
        return jnp.dot(hidden[None, :], w_expert_down[group_id], preferred_element_type=jnp.float32)[0].astype(jnp.bfloat16)
    expert_out = lax.map(expert_one, (moe_in, group_ids[:, 0], spread))
    dense_hidden = jax.nn.silu(jnp.dot(moe_in, w_dense_in, preferred_element_type=jnp.float32)).astype(jnp.bfloat16)
    dense_out = jnp.dot(dense_hidden, w_dense_out, preferred_element_type=jnp.float32)
    layer_output = residual.astype(jnp.float32) + expert_out.astype(jnp.float32) + jax.nn.sigmoid(dense_gate) * dense_out
    return (layer_output.astype(jnp.bfloat16), new_keys, new_values, new_gates)
```

```python
import functools
import jax
import jax.numpy as jnp
from jax import lax
from jax.experimental import pallas as pl
from jax.experimental.pallas import tpu as pltpu
from jax.sharding import PartitionSpec as P

FFE = 512
EPG = 4
EPS = 1e-06
FLOOR = -1e30
F32 = jnp.float32
BF16 = jnp.bfloat16
MESH = pl.DeviceIdType.MESH


def mm(a, b):
    return jnp.dot(a, b, preferred_element_type=F32)


def iota(shape, dim):
    return lax.broadcasted_iota(jnp.int32, shape, dim)


def norm_rows(values, gain):
    factor = lax.rsqrt(jnp.mean(values * values, axis=-1, keepdims=True) + EPS)
    return (values * factor * gain).astype(BF16)


def head_norm(values):
    factor = lax.rsqrt(jnp.mean(values * values, axis=-1, keepdims=True) + EPS)
    return (values * factor).astype(BF16)


def kernel(
    n_ep, n_tp, seqs, heads, head_dim, stored, cap, capacity,
    tokens, key_cache, value_cache, gate_totals, lengths, attn_gain,
    w_query, w_key, w_value, w_forget, forget_bias, w_attn_out, moe_gain,
    group_ids, inner_ids, group_prob, pair_logits,
    w_expert_gate, w_expert_up, w_expert_down, w_dense_in, w_dense_out, dense_gate,
    out, new_keys, new_values, new_gates,
    kbuf, vbuf, gbuf, wq, wk, wv, wo, wg, wu, wd, wdi, wdo,
    tok_all, part_send, part_recv, res_send, res_all, sel_send, row_recv,
    rw_send, rw_recv, dense_send, dense_recv, ret_send, ret_recv,
    k_sem, v_sem, w_sem,
    tok_s, tok_r, rw_s, rw_r, part_s, part_r, res_s, res_r, row_s, row_r,
    dn_s, dn_r, own_s, own_r, ret_s, ret_r,
):
    me_ep = lax.axis_index("ep")
    me_tp = lax.axis_index("tp")
    feat = tokens.shape[1]
    rows = seqs * heads
    per_group = 16 // heads
    n_groups = rows // 16

    def tp_peer(d):
        return lax.rem(me_tp + d, n_tp)

    def ep_peer(d):
        return lax.rem(me_ep + d, n_ep)

    def remote(src, dst, send, recv, ep, tp):
        return pltpu.make_async_remote_copy(
            src_ref=src, dst_ref=dst, send_sem=send, recv_sem=recv,
            device_id=(ep, tp), device_id_type=MESH,
        )

    local = []

    def load(src, dst, sem):
        copy = pltpu.make_async_copy(src, dst, sem)
        copy.start()
        return copy

    c_wq = load(w_query, wq, w_sem.at[0])
    c_wk = load(w_key, wk, w_sem.at[1])
    c_wv = load(w_value, wv, w_sem.at[2])
    c_gt = load(gate_totals, gbuf, w_sem.at[3])
    c_k = [load(key_cache.at[s], kbuf.at[s], k_sem.at[s]) for s in range(seqs)]
    c_v = [load(value_cache.at[s], vbuf.at[s], v_sem.at[s]) for s in range(seqs)]
    c_wo = load(w_attn_out, wo, w_sem.at[4])
    c_wdi = load(w_dense_in, wdi, w_sem.at[5])
    c_wdo = load(w_dense_out, wdo, w_sem.at[6])
    c_wg = load(w_expert_gate.at[0], wg, w_sem.at[7])
    c_wu = load(w_expert_up.at[0], wu, w_sem.at[8])
    c_wd = load(w_expert_down.at[0], wd, w_sem.at[9])

    barrier = pltpu.get_barrier_semaphore()
    total = n_ep * n_tp
    me = me_ep * n_tp + me_tp

    def greet(i, carry):
        other = lax.rem(me + i, total)
        pl.semaphore_signal(
            barrier, inc=1, device_id=(other // n_tp, lax.rem(other, n_tp)), device_id_type=MESH
        )
        return carry

    lax.fori_loop(1, total, greet, 0)

    eye = iota((seqs, seqs), 0) == iota((seqs, seqs), 1)
    gid_col = group_ids[...]
    gid_sq = jnp.broadcast_to(gid_col, (seqs, seqs))
    gid_row = jnp.sum(jnp.where(eye, gid_sq, 0).astype(F32), axis=0, keepdims=True).astype(jnp.int32)
    same = gid_sq == gid_row
    later = iota((seqs, seqs), 0) > iota((seqs, seqs), 1)
    sooner = iota((seqs, seqs), 0) < iota((seqs, seqs), 1)
    slot_col = jnp.sum(jnp.where(same & later, 1.0, 0.0), axis=1, keepdims=True).astype(jnp.int32)
    slot_row = jnp.sum(jnp.where(same & sooner, 1.0, 0.0), axis=0, keepdims=True).astype(jnp.int32)
    pos_col = gid_col * cap + slot_col
    pos_row = gid_row * cap + slot_row
    pick = jnp.where(iota((n_ep * cap, seqs), 0) == pos_row, 1.0, 0.0).astype(BF16)
    pick_own = jnp.where(iota((cap, seqs), 0) + me_ep * cap == pos_row, 1.0, 0.0).astype(BF16)
    put = jnp.where(iota((seqs, n_ep * cap), 1) == pos_col, 1.0, 0.0).astype(BF16)

    def column_of(row):
        return jnp.sum(jnp.where(eye, jnp.broadcast_to(row, (seqs, seqs)), 0.0), axis=1, keepdims=True)

    logits = pair_logits[...]
    first = jax.nn.sigmoid(logits[:, 0:1] - logits[:, 1:2])
    prob = column_of(group_prob[...])
    lane = iota((seqs, 128), 1)
    picked = inner_ids[...]
    spread = jnp.where(picked[:, 0:1] == lane, prob * first, 0.0) + jnp.where(
        picked[:, 1:2] == lane, prob * (1.0 - first), 0.0
    )
    routed = mm(pick, spread.astype(BF16))
    for e in range(n_ep):
        rw_send[e] = routed[e * cap:(e + 1) * cap].astype(BF16)
    rw_recv[me_ep] = mm(pick_own, spread.astype(BF16)).astype(BF16)
    tok_all[me_tp] = tokens[...]

    pl.semaphore_wait(barrier, total - 1)

    for d in range(1, n_tp):
        p = tp_peer(d)
        remote(tokens, tok_all.at[me_tp], tok_s.at[d], tok_r.at[me_tp], me_ep, p).start()
    for d in range(1, n_ep):
        e = ep_peer(d)
        remote(rw_send.at[e], rw_recv.at[me_ep], rw_s.at[d], rw_r.at[me_ep], e, me_tp).start()
    for d in range(1, n_tp):
        p = tp_peer(d)
        remote(tokens, tok_all.at[p], tok_s.at[d], tok_r.at[p], me_ep, p).wait_recv()

    x = jnp.concatenate([tok_all[t].astype(F32) for t in range(n_tp)], axis=1)
    normed = norm_rows(x, attn_gain[...])
    c_wq.wait()
    zq = mm(normed, wq[...])
    c_wk.wait()
    zk = mm(normed, wk[...])
    c_wv.wait()
    zv = mm(normed, wv[...])
    gate_pre = mm(normed, w_forget[...]) + forget_bias[...]
    log_gate = jnp.minimum(gate_pre, 0.0) - jnp.log1p(jnp.exp(-jnp.abs(gate_pre)))

    q_rows = k_rows = v_rows = jnp.zeros((rows, head_dim), F32)
    for h in range(heads):
        place = jnp.where(
            iota((rows, seqs), 0) == iota((rows, seqs), 1) * heads + h, 1.0, 0.0
        ).astype(BF16)
        cols = slice(h * head_dim, (h + 1) * head_dim)
        q_rows = q_rows + mm(place, head_norm(zq[:, cols]))
        k_rows = k_rows + mm(place, head_norm(zk[:, cols]))
        v_rows = v_rows + mm(place, zv[:, cols].astype(BF16))
    new_keys[...] = k_rows.astype(BF16)
    new_values[...] = v_rows.astype(BF16)

    n_heads = log_gate.shape[1]
    row_seq = iota((rows, n_heads), 0) // heads
    lg_rows = jnp.zeros((rows, n_heads), F32)
    for s in range(seqs):
        lg_rows = jnp.where(row_seq == s, log_gate[s:s + 1, :], lg_rows)
    row_head = me_tp * heads + lax.rem(iota((rows, n_heads), 0), heads)
    lg_rows = jnp.sum(
        jnp.where(iota((rows, n_heads), 1) == row_head, lg_rows, 0.0), axis=1, keepdims=True
    )
    len_rows = jnp.sum(
        jnp.where(
            iota((rows, seqs), 1) == iota((rows, seqs), 0) // heads,
            jnp.broadcast_to(lengths[...].astype(F32), (rows, seqs)), 0.0,
        ),
        axis=1, keepdims=True,
    ).astype(jnp.int32)

    c_gt.wait()
    scale = head_dim ** (-0.5)
    wide_row = iota((16, stored), 0)
    entry = iota((16, stored), 1)
    slim_row = iota((16, head_dim), 0)
    att_list, ng_list = [], []
    for g in range(n_groups):
        here = slice(g * 16, (g + 1) * 16)
        q = q_rows[here]
        q_low = q.astype(BF16)
        scores = jnp.zeros((16, stored), F32)
        totals = jnp.zeros((16, stored), F32)
        for j in range(per_group):
            s = g * per_group + j
            c_k[s].wait()
            block = kbuf[s].reshape(heads * stored, head_dim)
            product = lax.dot_general(
                q_low, block, (((1,), (1,)), ((), ())), preferred_element_type=F32
            )
            for h in range(heads):
                at = wide_row == j * heads + h
                scores = jnp.where(at, product[:, h * stored:(h + 1) * stored], scores)
                totals = jnp.where(at, gbuf[s, h:h + 1, :], totals)
        length = len_rows[here]
        last = jnp.sum(jnp.where(entry == length - 1, totals, 0.0), axis=1, keepdims=True)
        current = last + lg_rows[here]
        ng_list.append(current)
        live = entry < length
        scores = jnp.where(live, scores * scale + current - totals, FLOOR)
        own_score = jnp.sum(q * k_rows[here], axis=1, keepdims=True) * scale
        peak = jnp.maximum(jnp.max(scores, axis=1, keepdims=True), own_score)
        terms = jnp.where(live, jnp.exp(scores - peak), 0.0)
        own_term = jnp.exp(own_score - peak)
        denom = jnp.sum(terms, axis=1, keepdims=True) + own_term
        weights = (terms / denom).astype(BF16)
        own_weight = (own_term / denom).astype(BF16).astype(F32)
        att = jnp.zeros((16, head_dim), F32)
        for j in range(per_group):
            s = g * per_group + j
            c_v[s].wait()
            for h in range(heads):
                att = jnp.where(slim_row == j * heads + h, mm(weights, vbuf[s, h]), att)
        att_list.append(att + own_weight * v_rows[here])
    att_rows = jnp.concatenate(att_list, axis=0).astype(BF16) if n_groups > 1 else att_list[0].astype(BF16)
    ng_col = jnp.concatenate(ng_list, axis=0) if n_groups > 1 else ng_list[0]

    pieces = []
    for h in range(heads):
        place = jnp.where(
            iota((seqs, rows), 1) == iota((seqs, rows), 0) * heads + h, 1.0, 0.0
        ).astype(BF16)
        pieces.append(mm(place, att_rows))
    attended = (jnp.concatenate(pieces, axis=1) if heads > 1 else pieces[0]).astype(BF16)

    c_wo.wait()
    projected = mm(attended, wo[...])
    for t in range(n_tp):
        part_send[t] = projected[:, t * feat:(t + 1) * feat].astype(BF16)
    for d in range(1, n_tp):
        p = tp_peer(d)
        remote(part_send.at[p], part_recv.at[me_tp], part_s.at[d], part_r.at[me_tp], me_ep, p).start()
    part_recv[me_tp] = part_send[me_tp]

    ng_row = jnp.sum(
        jnp.where(iota((rows, rows), 0) == iota((rows, rows), 1), jnp.broadcast_to(ng_col, (rows, rows)), 0.0),
        axis=0, keepdims=True,
    )
    ng = jnp.zeros((seqs, heads), F32)
    for h in range(heads):
        col = jnp.sum(
            jnp.where(iota((seqs, rows), 1) == iota((seqs, rows), 0) * heads + h, ng_row, 0.0),
            axis=1, keepdims=True,
        )
        ng = jnp.where(iota((seqs, heads), 1) == h, col, ng)
    new_gates[...] = ng

    for d in range(1, n_tp):
        p = tp_peer(d)
        remote(part_send.at[p], part_recv.at[p], part_s.at[d], part_r.at[p], me_ep, p).wait_recv()
    summed = part_recv[0].astype(F32)
    for t in range(1, n_tp):
        summed = summed + part_recv[t].astype(F32)
    residual = (tokens[...].astype(F32) + summed).astype(BF16)

    res_send[...] = residual
    for d in range(1, n_tp):
        p = tp_peer(d)
        remote(res_send, res_all.at[me_tp], res_s.at[d], res_r.at[me_tp], me_ep, p).start()
    chosen = mm(pick, residual)
    for e in range(n_ep):
        sel_send[e] = chosen[e * cap:(e + 1) * cap].astype(BF16)
    for d in range(1, n_ep):
        e = ep_peer(d)

        def send_rows(i, carry, e=e, d=d):
            remote(
                sel_send.at[e], row_recv.at[me_ep, me_tp], row_s.at[d], row_r.at[me_ep], e, tp_peer(i)
            ).start()
            return carry

        lax.fori_loop(0, n_tp, send_rows, 0)
    res_all[me_tp] = residual

    for d in range(1, n_tp):
        p = tp_peer(d)
        remote(res_send, res_all.at[p], res_s.at[d], res_r.at[p], me_ep, p).wait_recv()
    res_full = jnp.concatenate([res_all[t].astype(F32) for t in range(n_tp)], axis=1)
    moe_in = norm_rows(res_full, moe_gain[...])
    own_rows = mm(pick_own, res_full.astype(BF16))
    for t in range(n_tp):
        row_recv[me_ep, t] = own_rows[:, t * feat:(t + 1) * feat].astype(BF16)

    c_wdi.wait()
    dense_hidden = jax.nn.silu(mm(moe_in, wdi[...])).astype(BF16)
    c_wdo.wait()
    dense_part = mm(dense_hidden, wdo[...])
    for t in range(n_tp):
        dense_send[t] = dense_part[:, t * feat:(t + 1) * feat].astype(BF16)
    for d in range(1, n_tp):
        p = tp_peer(d)
        remote(dense_send.at[p], dense_recv.at[me_tp], dn_s.at[d], dn_r.at[me_tp], me_ep, p).start()
    dense_recv[me_tp] = dense_send[me_tp]

    for d in range(1, n_ep):
        e = ep_peer(d)
        remote(rw_send.at[e], rw_recv.at[e], rw_s.at[d], rw_r.at[e], e, me_tp).wait_recv()
        remote(row_recv.at[e], row_recv.at[e], row_s.at[d], row_r.at[e], e, me_tp).wait_recv()
    gathered = jnp.concatenate(
        [
            jnp.concatenate([row_recv[e, t].astype(F32) for t in range(n_tp)], axis=1)
            for e in range(n_ep)
        ],
        axis=0,
    )
    expert_in = norm_rows(gathered, moe_gain[...])
    route = jnp.concatenate([rw_recv[e].astype(F32) for e in range(n_ep)], axis=0)
    expert_index = me_tp * w_expert_gate.shape[2] // FFE
    route_col = jnp.sum(
        jnp.where(iota(route.shape, 1) == expert_index, route, 0.0), axis=1, keepdims=True
    )
    c_wg.wait()
    gate_mid = mm(expert_in, wg[...])
    c_wu.wait()
    up_mid = mm(expert_in, wu[...])
    hidden = (jax.nn.silu(gate_mid) * up_mid * route_col).astype(BF16)
    c_wd.wait()
    expert_part = mm(hidden, wd[...])
    for e in range(n_ep):
        for t in range(n_tp):
            ret_send[e, t] = expert_part[e * cap:(e + 1) * cap, t * feat:(t + 1) * feat].astype(BF16)
    for d in range(1, n_ep):
        e = ep_peer(d)

        def send_back(i, carry, e=e, d=d):
            p = tp_peer(i)
            remote(
                ret_send.at[e, p], ret_recv.at[me_ep, me_tp], ret_s.at[d], ret_r.at[me_ep], e, p
            ).start()
            return carry

        lax.fori_loop(0, n_tp, send_back, 0)
    for d in range(1, n_tp):
        p = tp_peer(d)
        remote(
            ret_send.at[me_ep, p], ret_recv.at[me_ep, me_tp], own_s.at[d], own_r.at[me_tp], me_ep, p
        ).start()
    ret_recv[me_ep, me_tp] = ret_send[me_ep, me_tp]

    for d in range(1, n_tp):
        p = tp_peer(d)
        remote(dense_send.at[p], dense_recv.at[p], dn_s.at[d], dn_r.at[p], me_ep, p).wait_recv()
    dense_sum = dense_recv[0].astype(F32)
    for t in range(1, n_tp):
        dense_sum = dense_sum + dense_recv[t].astype(F32)
    base = residual.astype(F32) + jax.nn.sigmoid(dense_gate[...]) * dense_sum
    for d in range(1, n_tp):
        p = tp_peer(d)
        remote(
            ret_send.at[me_ep, p], ret_recv.at[me_ep, p], own_s.at[d], own_r.at[p], me_ep, p
        ).wait_recv()
    for d in range(1, n_ep):
        e = ep_peer(d)
        remote(ret_recv.at[e], ret_recv.at[e], ret_s.at[d], ret_r.at[e], e, me_tp).wait_recv()
    sums = []
    for e in range(n_ep):
        acc = ret_recv[e, 0].astype(F32)
        for t in range(1, n_tp):
            acc = acc + ret_recv[e, t].astype(F32)
        sums.append(acc)
    expert_out = mm(put, jnp.concatenate(sums, axis=0).astype(BF16))
    out[...] = (base + expert_out).astype(BF16)

    for d in range(1, n_tp):
        p = tp_peer(d)
        remote(tokens, tok_all.at[me_tp], tok_s.at[d], tok_r.at[me_tp], me_ep, p).wait_send()
        remote(part_send.at[p], part_recv.at[me_tp], part_s.at[d], part_r.at[me_tp], me_ep, p).wait_send()
        remote(res_send, res_all.at[me_tp], res_s.at[d], res_r.at[me_tp], me_ep, p).wait_send()
        remote(dense_send.at[p], dense_recv.at[me_tp], dn_s.at[d], dn_r.at[me_tp], me_ep, p).wait_send()
        remote(
            ret_send.at[me_ep, p], ret_recv.at[me_ep, me_tp], own_s.at[d], own_r.at[me_tp], me_ep, p
        ).wait_send()
    for d in range(1, n_ep):
        e = ep_peer(d)
        remote(rw_send.at[e], rw_recv.at[me_ep], rw_s.at[d], rw_r.at[me_ep], e, me_tp).wait_send()
        remote(row_recv.at[e], row_recv.at[e], row_s.at[d], row_r.at[e], e, me_tp).wait_send()
        remote(ret_recv.at[e], ret_recv.at[e], ret_s.at[d], ret_r.at[e], e, me_tp).wait_send()


def body(n_ep, n_tp, *args):
    (
        tokens, key_cache, value_cache, gate_totals, lengths, attn_gain,
        w_query, w_key, w_value, w_forget, forget_bias, w_attn_out, moe_gain,
        group_ids, inner_ids, group_prob, pair_logits,
        w_expert_gate, w_expert_up, w_expert_down, w_dense_in, w_dense_out, dense_gate,
    ) = args
    seqs, heads, stored, head_dim = key_cache.shape
    feat = tokens.shape[1]
    capacity = max(2, 2 * seqs // n_ep)
    cap = -(-capacity // 8) * 8
    rows = seqs * heads
    vm = pl.BlockSpec(memory_space=pltpu.VMEM)
    hb = pl.BlockSpec(memory_space=pl.ANY)

    def like(a):
        return pltpu.VMEM(a.shape, a.dtype)

    def dma(*n):
        return pltpu.SemaphoreType.DMA(n)

    operands = (
        tokens, key_cache, value_cache, gate_totals, lengths.reshape(1, -1), attn_gain.reshape(1, -1),
        w_query, w_key, w_value, w_forget, forget_bias.reshape(1, -1), w_attn_out,
        moe_gain.reshape(1, -1), group_ids, inner_ids, group_prob.reshape(1, -1), pair_logits,
        w_expert_gate, w_expert_up, w_expert_down, w_dense_in, w_dense_out, dense_gate.reshape(1, -1),
    )
    specs = [vm, hb, hb, hb, vm, vm, hb, hb, hb, vm, vm, hb, vm, vm, vm, vm, vm, hb, hb, hb, hb, hb, vm]
    scratch = [
        like(key_cache), like(value_cache), like(gate_totals),
        like(w_query), like(w_key), like(w_value), like(w_attn_out),
        pltpu.VMEM(w_expert_gate.shape[1:], BF16),
        pltpu.VMEM(w_expert_up.shape[1:], BF16),
        pltpu.VMEM(w_expert_down.shape[1:], BF16),
        like(w_dense_in), like(w_dense_out),
        pltpu.VMEM((n_tp, seqs, feat), BF16),
        pltpu.VMEM((n_tp, seqs, feat), BF16),
        pltpu.VMEM((n_tp, seqs, feat), BF16),
        pltpu.VMEM((seqs, feat), BF16),
        pltpu.VMEM((n_tp, seqs, feat), BF16),
        pltpu.VMEM((n_ep, cap, feat), BF16),
        pltpu.VMEM((n_ep, n_tp, cap, feat), BF16),
        pltpu.VMEM((n_ep, cap, 128), BF16),
        pltpu.VMEM((n_ep, cap, 128), BF16),
        pltpu.VMEM((n_tp, seqs, feat), BF16),
        pltpu.VMEM((n_tp, seqs, feat), BF16),
        pltpu.VMEM((n_ep, n_tp, cap, feat), BF16),
        pltpu.VMEM((n_ep, n_tp, cap, feat), BF16),
        dma(seqs), dma(seqs), dma(10),
        dma(n_tp), dma(n_tp), dma(n_ep), dma(n_ep), dma(n_tp), dma(n_tp),
        dma(n_tp), dma(n_tp), dma(n_ep), dma(n_ep),
        dma(n_tp), dma(n_tp), dma(n_tp), dma(n_tp), dma(n_ep), dma(n_ep),
    ]
    out, keys, values, gates = pl.pallas_call(
        functools.partial(kernel, n_ep, n_tp, seqs, heads, head_dim, stored, cap, capacity),
        out_shape=(
            jax.ShapeDtypeStruct((seqs, feat), BF16),
            jax.ShapeDtypeStruct((rows, head_dim), BF16),
            jax.ShapeDtypeStruct((rows, head_dim), BF16),
            jax.ShapeDtypeStruct((seqs, heads), F32),
        ),
        in_specs=specs,
        out_specs=(vm, vm, vm, vm),
        scratch_shapes=scratch,
        compiler_params=pltpu.CompilerParams(
            collective_id=0, has_side_effects=True, vmem_limit_bytes=56 * 1024 * 1024
        ),
    )(*operands)
    shape = (seqs, heads, head_dim)
    return out, keys.reshape(shape), values.reshape(shape), gates


def solution(mesh):
    placed = (
        P("ep", "tp"),
        P("ep", "tp", None, None),
        P("ep", "tp", None, None),
        P("ep", "tp", None),
        P("ep"),
        P(),
        P(None, "tp"),
        P(None, "tp"),
        P(None, "tp"),
        P(),
        P(),
        P("tp", None),
        P(),
        P("ep", None),
        P("ep", None),
        P("ep"),
        P("ep", None),
        P("ep", None, "tp"),
        P("ep", None, "tp"),
        P("ep", "tp", None),
        P(None, "tp"),
        P("tp", None),
        P("tp"),
    )
    return jax.shard_map(
        functools.partial(body, mesh.shape["ep"], mesh.shape["tp"]),
        mesh=mesh,
        in_specs=placed,
        out_specs=(P("ep", "tp"), P("ep", "tp", None), P("ep", "tp", None), P("ep", "tp")),
        check_vma=False,
    )
```
